32 devices in a mesh: gr: 2 (over x), sp: 8 (over z, y), tp: 2 (over core).
Axes of the slice: x: 2, y: 2, z: 4, core: 2. Of those that a mesh axis runs over, the one named last changes fastest.
Arguments:
- inputs: bfloat16 [4096, 2048], P(('gr', 'sp'), 'tp'), parts along dimension 0, may hold values from -6 to 6
- x_weight: bfloat16 [2048, 4096], P(None, 'tp'), may hold values from -0.125 to 0.125
- b_weight: bfloat16 [2048, 2048], P(None, 'tp'), may hold values from -0.125 to 0.125
- dt_weight: bfloat16 [2048, 128], replicated, may hold values from -0.125 to 0.125
- dt_bias: float32 [2, 64], replicated, may hold values from -2 to -1
- decay_rate: float32 [2, 64], replicated, may hold values from 0.3 to 10
- conv_x: bfloat16 [5, 4096], P(None, 'tp'), may hold values from -2.5 to 2.5
- conv_b: bfloat16 [5, 2048], P(None, 'tp'), may hold values from -2.5 to 2.5
- query_c: bfloat16 [2, 16, 128], P('gr', 'tp'), parts along dimension 0, may hold values from -6 to 6
- query_gate: bfloat16 [2, 64, 64], P('gr', 'tp'), parts along dimension 0, may hold values from -6 to 6
- read_span: int32 [2], P('gr'), parts along dimension 0, may hold values from 0 to 15
- read_gain: float32 [64, 64], P('tp'), may hold values from 0.1 to 1.9
Outputs:
- span_cache: bfloat16 [32, 2, 64, 8192], P('gr', None, 'tp', 'sp'), parts along dimension 0
- first_read: bfloat16 [2, 64, 64], P('gr', 'tp'), parts along dimension 0
The draws below stay inside these ranges and needn't reach their ends.
There are 2 independent parts, one for each index of `gr`. The reference program is written for one: setup_inputs(seed, part) draws one part's arguments, and reference() takes and returns one part's arrays. A program takes and returns all parts, laid end to end along the dimension named above; an argument that names none is the same for every part. Nothing has to cross between parts.
Inputs may be any that keep to these rules, and one draw needn't show every extreme that they name: read_span holds one span index from 0 to 15.
All inputs are finite; a program needn't handle non-finite values.
Results may differ from the reference program's by a relative error of at most 0.009.
Values may be sent and summed in bfloat16 or wider, within the bound.
A program may use at most 64 MiB of HBM per device.

```python
import math
import jax
import jax.numpy as jnp
from jax import lax

D = 2048
H = 64
P_SIZE = 64
G = 16
N = 128
KW = 5
SPAN = 128
LEN = 2048
SPANS = 16


def levels(rng, extent, shards, least, high):
    def one(dim, parts):
        heights = jax.random.uniform(jax.random.fold_in(jax.random.fold_in(rng, 6), dim), (parts,), jnp.float32, least / len(shards), high / len(shards))
        return jnp.repeat(jnp.exp(heights), extent[dim] // parts).reshape((-1,) + (1,) * (len(extent) - dim - 1))

    level = one(*shards[0])
    for cut in shards[1:]:
        level = level * one(*cut)
    return level


def gaussian(rng, extent, width, limit, split=(), kind=jnp.bfloat16):
    entries = jax.random.normal(rng, extent, jnp.float32) * width
    if len(split) > 0:
        entries = levels(rng, extent, split, -0.22, 0.18) * entries
    return jnp.clip(entries, min=-limit, max=limit).astype(kind)


def setup_inputs(seed: int = 0, part: int = 0) -> dict:
    arg_keys = jax.random.split(jax.random.key(seed), 13)
    part_keys = jax.random.split(jax.random.fold_in(arg_keys[12], part), 13)
    return {
        "inputs": gaussian(part_keys[0], (LEN, D), 1.0, 6.0, ((0, 8), (1, 2))),
        "x_weight": gaussian(arg_keys[1], (D, H * P_SIZE), D ** -0.5, 0.125, ((1, 2),)),
        "b_weight": gaussian(arg_keys[2], (D, G * N), D ** -0.5, 0.125, ((1, 2),)),
        "dt_weight": gaussian(arg_keys[3], (D, 2 * H), D ** -0.5, 0.125),
        "dt_bias": jnp.clip(jax.random.uniform(arg_keys[4], (2, H), jnp.float32, -2.0, -1.0), -2.0, -1.0),
        "decay_rate": jnp.clip(jnp.exp(jax.random.uniform(arg_keys[5], (2, H), jnp.float32, math.log(0.3), math.log(10.0))), 0.3, 10.0),
        "conv_x": gaussian(arg_keys[6], (KW, H * P_SIZE), KW ** -0.5, 2.5, ((1, 2),)),
        "conv_b": gaussian(arg_keys[7], (KW, G * N), KW ** -0.5, 2.5, ((1, 2),)),
        "query_c": gaussian(part_keys[8], (1, G, N), 1.0, 6.0, ((1, 2),)),
        "query_gate": gaussian(part_keys[9], (1, H, P_SIZE), 1.0, 6.0, ((1, 2),)),
        "read_span": jax.random.randint(part_keys[10], (1,), 0, SPANS).astype(jnp.int32),
        "read_gain": jnp.clip(1.0 + 0.18 * jax.random.normal(arg_keys[11], (H, P_SIZE), jnp.float32), 0.1, 1.9),
    }


EPSILON = 1e-06

def conv_silu(projected, taps):
    kernel = taps.shape[0]
    reach = kernel // 2
    length = projected.shape[0]
    padded = jnp.pad(projected.astype(jnp.float32), ((reach, reach), (0, 0)))
    result = jnp.zeros((length, projected.shape[1]), jnp.float32)
    for offset in range(kernel):
        result = result + taps[offset].astype(jnp.float32) * padded[offset:offset + length]
    return jax.nn.silu(result).astype(jnp.bfloat16)

def span_states(value_rows, key_rows, step_sizes, log_decay):
    running = jnp.cumsum(log_decay, axis=1)
    closing = running[:, -1]
    forward = jnp.exp(closing[:, None, 0] - running[:, :, 0]) * step_sizes[:, :, 0]
    backward = jnp.exp(running[:, :, 1] - log_decay[:, :, 1]) * step_sizes[:, :, 1]
    weights = jnp.stack([forward, backward], axis=2)
    states = jnp.einsum('kseh,kshn,kshp->kehnp', weights, key_rows.astype(jnp.float32), value_rows.astype(jnp.float32))
    return (states, closing)

def read_weights(span_logs, chosen):
    span_count = span_logs.shape[0]
    ahead_sum = jnp.cumsum(span_logs[:, 0], axis=0)
    behind = jnp.flip(jnp.cumsum(jnp.flip(span_logs[:, 1], 0), axis=0), 0)
    positions = jnp.arange(span_count, dtype=jnp.int32)[:, None]
    ahead_pick = lax.dynamic_slice_in_dim(ahead_sum, chosen, 1, 0)
    behind_pick = lax.dynamic_slice_in_dim(behind, chosen, 1, 0)
    before = positions <= chosen
    after = positions >= chosen
    forward = jnp.where(before, jnp.exp(jnp.where(before, ahead_pick - ahead_sum, 0.0)), 0.0)
    backward = jnp.where(after, jnp.exp(jnp.where(after, behind_pick - behind, 0.0)), 0.0)
    return jnp.stack([forward, backward], axis=1)

def reference(inputs, x_weight, b_weight, dt_weight, dt_bias, decay_rate, conv_x, conv_b, query_c, query_gate, read_span, read_gain):
    length = inputs.shape[0]
    values = conv_silu(jnp.dot(inputs, x_weight, preferred_element_type=jnp.float32).astype(jnp.bfloat16), conv_x)
    key_rows = conv_silu(jnp.dot(inputs, b_weight, preferred_element_type=jnp.float32).astype(jnp.bfloat16), conv_b)
    dt_raw = jnp.dot(inputs, dt_weight, preferred_element_type=jnp.float32).astype(jnp.bfloat16).reshape(length, 2, H)
    step_sizes = jax.nn.softplus(dt_raw.astype(jnp.float32) + dt_bias)
    log_decay = -(step_sizes * decay_rate) / length
    span_count = length // SPAN
    step_sizes = step_sizes.reshape(span_count, SPAN, 2, H)
    log_decay = log_decay.reshape(span_count, SPAN, 2, H)
    span_logs = lax.optimization_barrier(jnp.sum(log_decay, axis=1))
    weights = read_weights(span_logs, read_span[0])
    per_group = H // G

    def one_group(group_index):
        first_head = group_index * per_group
        group_values = lax.dynamic_slice_in_dim(values, first_head * P_SIZE, per_group * P_SIZE, 1).reshape(span_count, SPAN, per_group, P_SIZE)
        group_keys = lax.dynamic_slice_in_dim(key_rows, group_index * N, N, 1).reshape(span_count, SPAN, 1, N)
        group_keys = jnp.broadcast_to(group_keys, (span_count, SPAN, per_group, N))
        group_steps = lax.dynamic_slice_in_dim(step_sizes, first_head, per_group, 3)
        group_logs = lax.dynamic_slice_in_dim(log_decay, first_head, per_group, 3)
        states, unused = span_states(group_values, group_keys, group_steps, group_logs)
        row_block = states.reshape(span_count, 2, per_group, N * P_SIZE).astype(jnp.bfloat16)
        group_weights = lax.dynamic_slice_in_dim(weights, first_head, per_group, 2)
        gathered = jnp.einsum('jeh,jehx->hx', group_weights, row_block.astype(jnp.float32))
        return (row_block, gathered)
    row_block, gathered = lax.map(one_group, jnp.arange(G, dtype=jnp.int32))
    span_cache = jnp.transpose(row_block, (1, 2, 0, 3, 4)).reshape(span_count, 2, H, N * P_SIZE)
    read_state = gathered.reshape(H, N, P_SIZE)
    query_cols = jnp.repeat(query_c[0].astype(jnp.float32), per_group, axis=0)
    read_total = jnp.einsum('hnp,hn->hp', read_state, query_cols)
    gated_read = read_total * jax.nn.silu(query_gate[0].astype(jnp.float32))
    mean_square = jnp.mean(gated_read * gated_read)
    first_read = (gated_read * lax.rsqrt(mean_square + EPSILON) * read_gain)[None].astype(jnp.bfloat16)
    return (span_cache, first_read)
```

```python
import functools

import jax
import jax.numpy as jnp
from jax import lax
from jax.experimental import pallas as pl
from jax.experimental.pallas import tpu as pltpu
from jax.sharding import PartitionSpec as P

H = 64
P_SIZE = 64
G = 16
N = 128
KW = 5
SPAN = 128
EPSILON = 1e-06
PER = H // G
EDGE = 16
ROWS = 16
PITCH = N + 8
LANES = 128
MESH = pl.DeviceIdType.MESH
F32 = jnp.float32
BF16 = jnp.bfloat16


def conv_silu(projected, taps, tokens):
    rounded = projected.astype(BF16).astype(F32)
    total = rounded.shape[0]
    reach = KW // 2
    mixed = None
    for k in range(KW):
        shift = (reach - k) % total
        moved = rounded if shift == 0 else pltpu.roll(rounded, shift, 0)
        term = taps[k : k + 1] * moved[EDGE : EDGE + tokens]
        mixed = term if mixed is None else mixed + term
    return (mixed / (1.0 + jnp.exp(-mixed))).astype(BF16).astype(F32)


def kernel(
    n, width, x, xw, bw, dtw, bias, rate, cx, cb, q, gate, chosen, gain,
    out, fr,
    xext, xwv, bwv, held, stage, wts, reads, qcol, logs, parts, squares,
    sem_w, sem_own, sem_x, sem_halo, sem_c, sem_y, sem_big, sem_self, sem_sq,
):
    s = lax.axis_index("sp")
    c = lax.axis_index("tp")
    tokens, feats = x.shape
    spans = tokens // SPAN
    heads = xw.shape[1] // P_SIZE
    groups = heads // PER
    tile = min(ROWS, heads)
    blocks = heads // tile
    vcols = PER * P_SIZE
    columns = stage.shape[-1]
    lane = lax.broadcasted_iota(jnp.int32, (1, LANES), 1)
    low = lane < P_SIZE

    def peer(k):
        return lax.rem(s + k, n)

    def mate(k):
        return lax.rem(c + k, width)

    def weight_copies(j):
        at_x = pl.ds(pl.multiple_of(j * vcols, vcols), vcols)
        at_b = pl.ds(pl.multiple_of(j * N, N), N)
        return (
            pltpu.make_async_copy(xw.at[:, at_x], xwv.at[:, at_x], sem_w.at[0, j]),
            pltpu.make_async_copy(bw.at[:, at_b], bwv.at[:, at_b], sem_w.at[1, j]),
        )

    for j in range(groups):
        for copy in weight_copies(j):
            copy.start()
    mine = pl.ds(pl.multiple_of(c * feats, feats), feats)
    own = pltpu.make_async_copy(x, xext.at[pl.ds(EDGE, tokens), mine], sem_own)
    own.start()

    barrier = pltpu.get_barrier_semaphore()

    @pl.loop(1, n)
    def _(k):
        pl.semaphore_signal(barrier, inc=1, device_id={"sp": peer(k), "tp": c}, device_id_type=MESH)

    @pl.loop(1, width)
    def _(k):
        pl.semaphore_signal(barrier, inc=1, device_id={"sp": s, "tp": mate(k)}, device_id_type=MESH)

    @pl.when(s > 0)
    def _():
        @pl.loop(1, width)
        def _(k):
            pl.semaphore_signal(
                barrier, inc=1, device_id={"sp": s - 1, "tp": mate(k)}, device_id_type=MESH
            )

    @pl.when(s < n - 1)
    def _():
        @pl.loop(1, width)
        def _(k):
            pl.semaphore_signal(
                barrier, inc=1, device_id={"sp": s + 1, "tp": mate(k)}, device_id_type=MESH
            )

    @pl.when(s == 0)
    def _():
        xext[pl.ds(0, EDGE), :] = jnp.zeros((EDGE, xext.shape[1]), BF16)

    @pl.when(s == n - 1)
    def _():
        xext[pl.ds(EDGE + tokens, EDGE), :] = jnp.zeros((EDGE, xext.shape[1]), BF16)

    sides = lax.min(s, 1) + lax.min(n - 1 - s, 1)
    pl.semaphore_wait(barrier, n - 1 + (width - 1) * (1 + sides))

    def swap(k):
        return pltpu.make_async_remote_copy(
            src_ref=x,
            dst_ref=xext.at[pl.ds(EDGE, tokens), mine],
            send_sem=sem_x.at[0, k],
            recv_sem=sem_x.at[1, k],
            device_id={"sp": s, "tp": mate(k)},
            device_id_type=MESH,
        )

    for k in range(1, width):
        swap(k).start()

    def halo(up, cross):
        slot = width * up + cross
        return pltpu.make_async_remote_copy(
            src_ref=x.at[pl.ds(tokens - EDGE if up else 0, EDGE), :],
            dst_ref=xext.at[pl.ds(0 if up else EDGE + tokens, EDGE), mine],
            send_sem=sem_halo.at[0, slot],
            recv_sem=sem_halo.at[1, slot],
            device_id={"sp": s + 1 if up else s - 1, "tp": mate(cross)},
            device_id_type=MESH,
        )

    @pl.when(s < n - 1)
    def _():
        for k in range(width):
            halo(1, k).start()

    @pl.when(s > 0)
    def _():
        for k in range(width):
            halo(0, k).start()

    turned = jnp.transpose(q[0].astype(F32))
    for g in range(groups):
        qcol[g] = jnp.broadcast_to(turned[:, g : g + 1], (N, LANES))

    own.wait()
    for k in range(1, width):
        swap(k).wait_recv()

    raw = jnp.dot(xext[pl.ds(EDGE, tokens), :], dtw[...], preferred_element_type=F32)
    offset = jnp.concatenate([bias[0:1, :], bias[1:2, :]], axis=1)
    speed = jnp.concatenate([rate[0:1, :], rate[1:2, :]], axis=1)
    raw = raw.astype(BF16).astype(F32) + offset
    step = jnp.maximum(raw, 0.0) + jnp.log1p(jnp.exp(-jnp.abs(raw)))
    decay = -(step * speed) / (tokens * n)
    row = lax.broadcasted_iota(jnp.int32, (SPAN, SPAN), 0)
    col = lax.broadcasted_iota(jnp.int32, (SPAN, SPAN), 1)
    later = jnp.where(col > row, 1.0, 0.0).astype(F32)
    earlier = jnp.where(col < row, 1.0, 0.0).astype(F32)
    local = lax.rem(2 * H - c * heads, 2 * H)
    sub = lax.broadcasted_iota(jnp.int32, (8, LANES), 0)
    closing = jnp.zeros((8, LANES), F32)
    for j in range(spans):
        piece = decay[j * SPAN : (j + 1) * SPAN]
        ahead = jnp.dot(later, piece, precision=lax.Precision.HIGHEST, preferred_element_type=F32)
        behind = jnp.dot(earlier, piece, precision=lax.Precision.HIGHEST, preferred_element_type=F32)
        weight = jnp.exp(jnp.where(low, ahead, behind)) * step[j * SPAN : (j + 1) * SPAN]
        wts[j] = pltpu.roll(weight, local, 1)
        closing = jnp.where(sub == j, jnp.sum(piece, axis=0, keepdims=True), closing)
    logs[s] = closing

    def log_copy(k):
        return pltpu.make_async_remote_copy(
            src_ref=logs.at[s],
            dst_ref=logs.at[s],
            send_sem=sem_c.at[0, k],
            recv_sem=sem_c.at[1, k],
            device_id={"sp": peer(k), "tp": c},
            device_id_type=MESH,
        )

    @pl.loop(1, n)
    def _(k):
        log_copy(k).start()

    @pl.when(s > 0)
    def _():
        for k in range(width):
            halo(1, k).wait_recv()

    @pl.when(s < n - 1)
    def _():
        for k in range(width):
            halo(0, k).wait_recv()

    def one_group(block, i):
        j = block * (tile // PER) + i
        for copy in weight_copies(j):
            copy.wait()
        at_x = pl.ds(pl.multiple_of(j * vcols, vcols), vcols)
        at_b = pl.ds(pl.multiple_of(j * N, N), N)
        rows = xext[...]
        keys = conv_silu(
            jnp.dot(rows, bwv[:, at_b], preferred_element_type=F32), cb[:, at_b].astype(F32), tokens
        )
        values = conv_silu(
            jnp.dot(rows, xwv[:, at_x], preferred_element_type=F32), cx[:, at_x].astype(F32), tokens
        )
        back = lax.rem(LANES - j * PER, LANES)
        for k in range(spans):
            part = slice(k * SPAN, (k + 1) * SPAN)
            turned_keys = jnp.transpose(keys[part]).astype(BF16)
            weight = pltpu.roll(wts[k], back, 1)
            scaled = []
            for h in range(PER):
                pair = values[part, (h // 2) * LANES : (h // 2 + 1) * LANES]
                other = pltpu.roll(pair, P_SIZE, 1)
                doubled = jnp.where(low, pair, other) if h % 2 == 0 else jnp.where(low, other, pair)
                both = jnp.where(low, weight[:, h : h + 1], weight[:, H + h : H + h + 1])
                scaled.append((doubled * both).astype(BF16))
            states = jnp.dot(
                turned_keys, jnp.concatenate(scaled, axis=1), preferred_element_type=F32
            )
            for h in range(PER):
                state = states[:, h * LANES : (h + 1) * LANES]
                held[k, pl.ds(pl.multiple_of((i * PER + h) * PITCH, 8), N), :] = state
                seen = jnp.sum(qcol[j] * state.astype(BF16).astype(F32), axis=0, keepdims=True)
                reads[k, pl.ds(j * PER + h, 1), :] = seen

    def big_copy(block, k):
        at = pl.ds(block * tile, tile)
        return pltpu.make_async_remote_copy(
            src_ref=stage.at[peer(k), :, :, at, :],
            dst_ref=out.at[pl.ds(s * spans, spans), :, at, :],
            send_sem=sem_big.at[0, block, k],
            recv_sem=sem_big.at[1, block, k],
            device_id={"sp": peer(k), "tp": c},
            device_id_type=MESH,
        )

    def self_copy(block):
        at = pl.ds(block * tile, tile)
        return pltpu.make_async_copy(
            stage.at[s, :, :, at, :], out.at[pl.ds(s * spans, spans), :, at, :], sem_self.at[block]
        )

    def lay_out(block, d):
        for k in range(spans):
            for m in range(columns // LANES):
                first = d * (columns // P_SIZE) + 2 * m
                even = held[k, pl.ds(first, tile, stride=PITCH), :]
                odd = held[k, pl.ds(first + 1, tile, stride=PITCH), :]
                at = pl.ds(m * LANES, LANES)
                stage[d, k, 0, pl.ds(block * tile, tile), at] = jnp.where(
                    low, even, pltpu.roll(odd, P_SIZE, 1)
                ).astype(BF16)
                stage[d, k, 1, pl.ds(block * tile, tile), at] = jnp.where(
                    low, pltpu.roll(even, P_SIZE, 1), odd
                ).astype(BF16)

    def part_copy(k):
        return pltpu.make_async_remote_copy(
            src_ref=parts.at[s],
            dst_ref=parts.at[s],
            send_sem=sem_y.at[0, k],
            recv_sem=sem_y.at[1, k],
            device_id={"sp": peer(k), "tp": c},
            device_id_type=MESH,
        )

    def send_read():
        @pl.loop(1, n)
        def _(k):
            log_copy(k).wait_recv()

        every = logs[...]
        index = lax.broadcasted_iota(jnp.int32, every.shape, 0) * spans + lax.broadcasted_iota(
            jnp.int32, every.shape, 1
        )
        real = lax.broadcasted_iota(jnp.int32, every.shape, 1) < spans
        r = chosen[0]
        table = jnp.zeros((8, LANES), F32)
        for k in range(spans):
            j = s * spans + k
            forward = real & (index > j) & (index <= r) & low[None]
            backward = real & (index < j) & (index >= r) & (~low)[None]
            total = jnp.sum(jnp.where(forward | backward, every, 0.0), axis=0)
            total = jnp.sum(total, axis=0, keepdims=True)
            ahead_on = jnp.where(j <= r, 1.0, 0.0)
            behind_on = jnp.where(j >= r, 1.0, 0.0)
            found = jnp.exp(total) * jnp.where(low, ahead_on, behind_on)
            table = jnp.where(sub == k, found, table)
        table = jnp.transpose(pltpu.roll(table, local, 1))
        sums = jnp.zeros((heads, LANES), F32)
        for k in range(spans):
            spread = jnp.where(low, table[0:heads, k : k + 1], table[H : H + heads, k : k + 1])
            sums = sums + spread * reads[k]
        parts[s] = sums

        @pl.loop(1, n)
        def _(k):
            part_copy(k).start()

    for block in range(blocks):

        @pl.loop(0, tile // PER)
        def _(i, block=block):
            one_group(block, i)

        if block == blocks - 1:
            send_read()

        @pl.loop(1, n)
        def _(k, block=block):
            lay_out(block, peer(k))
            big_copy(block, k).start()

        lay_out(block, s)
        self_copy(block).start()

    @pl.loop(1, n)
    def _(k):
        part_copy(k).wait_recv()

    def add_part(i, total):
        return total + parts[i]

    total = lax.fori_loop(1, n, add_part, parts[0])
    total = total + pltpu.roll(total, P_SIZE, 1)
    door = gate[0].astype(F32)
    gated = total[:, :P_SIZE] * (door / (1.0 + jnp.exp(-door)))
    squares[c] = jnp.broadcast_to(jnp.sum(gated * gated, keepdims=True), (8, LANES))

    def square(k):
        return pltpu.make_async_remote_copy(
            src_ref=squares.at[c],
            dst_ref=squares.at[c],
            send_sem=sem_sq.at[0, k],
            recv_sem=sem_sq.at[1, k],
            device_id={"sp": s, "tp": mate(k)},
            device_id_type=MESH,
        )

    for k in range(1, width):
        square(k).start()
    for k in range(1, width):
        square(k).wait_recv()
    mean = jnp.sum(squares[...], axis=0)[0:1, 0:1] / (H * P_SIZE)
    fr[0] = (gated * lax.rsqrt(mean + EPSILON) * gain[...]).astype(BF16)

    for k in range(1, width):
        square(k).wait_send()
    for k in range(1, width):
        swap(k).wait_send()

    @pl.when(s < n - 1)
    def _():
        for k in range(width):
            halo(1, k).wait_send()

    @pl.when(s > 0)
    def _():
        for k in range(width):
            halo(0, k).wait_send()

    @pl.loop(1, n)
    def _(k):
        log_copy(k).wait_send()
        part_copy(k).wait_send()

    for block in range(blocks):
        self_copy(block).wait()

        @pl.loop(1, n)
        def _(k, block=block):
            big_copy(block, k).wait()


def per_device(x, xw, bw, dtw, bias, rate, cx, cb, q, gate, chosen, gain):
    n = lax.axis_size("sp")
    width = lax.axis_size("tp")
    tokens, feats = x.shape
    depth = xw.shape[0]
    spans = tokens // SPAN
    heads = xw.shape[1] // P_SIZE
    groups = heads // PER
    tile = min(ROWS, heads)
    blocks = heads // tile
    columns = N * P_SIZE // n
    vmem = pl.BlockSpec(memory_space=pltpu.VMEM)
    anywhere = pl.BlockSpec(memory_space=pl.ANY)
    dma = pltpu.SemaphoreType.DMA
    return pl.pallas_call(
        functools.partial(kernel, n, width),
        out_shape=(
            jax.ShapeDtypeStruct((spans * n, 2, heads, columns), BF16),
            jax.ShapeDtypeStruct((1, heads, P_SIZE), BF16),
        ),
        in_specs=[vmem, anywhere, anywhere] + [vmem] * 7
        + [pl.BlockSpec(memory_space=pltpu.SMEM), vmem],
        out_specs=(vmem, vmem),
        scratch_shapes=[
            pltpu.VMEM((tokens + 2 * EDGE, depth), BF16),
            pltpu.VMEM(xw.shape, BF16),
            pltpu.VMEM(bw.shape, BF16),
            pltpu.VMEM((spans, tile * PITCH, LANES), F32),
            pltpu.VMEM((n, spans, 2, heads, columns), BF16),
            pltpu.VMEM((spans, SPAN, LANES), F32),
            pltpu.VMEM((spans, heads, LANES), F32),
            pltpu.VMEM((groups, N, LANES), F32),
            pltpu.VMEM((n, 8, LANES), F32),
            pltpu.VMEM((n, heads, LANES), F32),
            pltpu.VMEM((width, 8, LANES), F32),
            dma((2, groups)),
            dma,
            dma((2, width)),
            dma((2, 2 * width)),
            dma((2, n)),
            dma((2, n)),
            dma((2, blocks, n)),
            dma((blocks,)),
            dma((2, width)),
        ],
        compiler_params=pltpu.CompilerParams(
            collective_id=0, has_side_effects=True, vmem_limit_bytes=48 * 1024 * 1024
        ),
    )(x, xw, bw, dtw, bias, rate, cx, cb, q, gate, chosen, gain)


def solution(mesh):
    return jax.shard_map(
        per_device,
        mesh=mesh,
        in_specs=(
            P(("gr", "sp"), "tp"),
            P(None, "tp"),
            P(None, "tp"),
            P(),
            P(),
            P(),
            P(None, "tp"),
            P(None, "tp"),
            P("gr", "tp", None),
            P("gr", "tp", None),
            P("gr"),
            P("tp", None),
        ),
        out_specs=(P("gr", None, "tp", "sp"), P("gr", "tp", None)),
        check_vma=False,
    )
```

```python
import functools

import jax
import jax.numpy as jnp
from jax import lax
from jax.experimental import pallas as pl
from jax.experimental.pallas import tpu as pltpu
from jax.sharding import PartitionSpec as P

H = 64
P_SIZE = 64
G = 16
N = 128
KW = 5
SPAN = 128
EPSILON = 1e-06
PER = H // G
EDGE = 16
ROWS = 8
HALF = N // 2
PITCH = HALF + 8
LANES = 128
MESH = pl.DeviceIdType.MESH
F32 = jnp.float32
BF16 = jnp.bfloat16


def conv_silu(projected, taps, tokens):
    rounded = projected.astype(BF16).astype(F32)
    total = rounded.shape[0]
    reach = KW // 2
    mixed = None
    for k in range(KW):
        shift = (reach - k) % total
        moved = rounded if shift == 0 else pltpu.roll(rounded, shift, 0)
        term = taps[k : k + 1] * moved[EDGE : EDGE + tokens]
        mixed = term if mixed is None else mixed + term
    return (mixed / (1.0 + jnp.exp(-mixed))).astype(BF16).astype(F32)


def kernel(
    n, width, x, xw, bw, dtw_h, bias_h, rate_h, cx_h, cb_h, q_h, gate_h, chosen, gain_h,
    out, fr,
    dtw, bias, rate, cx, cb, q, gate, gain,
    xext, xwv, bwv, held, stage, wts, reads, qcol, logs, parts, squares,
    sem_small, sem_w, sem_own, sem_x, sem_far, sem_pass, sem_halo, sem_c, sem_y, sem_big, sem_self, sem_sq,
):
    s = lax.axis_index("sp")
    c = lax.axis_index("tp")
    tokens, feats = x.shape
    spans = tokens // SPAN
    heads = xw.shape[1] // P_SIZE
    groups = heads // PER
    tile = min(ROWS, heads)
    blocks = heads // tile
    vcols = PER * P_SIZE
    columns = stage.shape[-1]
    lane = lax.broadcasted_iota(jnp.int32, (1, LANES), 1)
    low = lane < P_SIZE

    half = n // 2
    side = s // half
    place = lax.rem(s, half)
    across = lax.rem(s + half, n)
    owners = (s, across)

    def peer(k):
        return lax.rem(s + k, n)

    def near(k):
        return lax.rem(place + k, half)

    def mate(k):
        return lax.rem(c + k, width)

    def weight_copies(j):
        at_x = pl.ds(pl.multiple_of(j * vcols, vcols), vcols)
        at_b = pl.ds(pl.multiple_of(j * N, N), N)
        return (
            pltpu.make_async_copy(xw.at[:, at_x], xwv.at[:, at_x], sem_w.at[0, j]),
            pltpu.make_async_copy(bw.at[:, at_b], bwv.at[:, at_b], sem_w.at[1, j]),
        )

    smalls = [
        pltpu.make_async_copy(a, b, sem_small.at[i])
        for i, (a, b) in enumerate(
            (
                (dtw_h, dtw), (bias_h, bias), (rate_h, rate), (cx_h, cx),
                (cb_h, cb), (q_h, q), (gate_h, gate), (gain_h, gain),
            )
        )
    ]
    mine = pl.ds(pl.multiple_of(c * feats, feats), feats)
    own = pltpu.make_async_copy(x, xext.at[0, pl.ds(EDGE, tokens), mine], sem_own)
    own.start()
    for copy in smalls:
        copy.start()
    for j in range(groups):
        for copy in weight_copies(j):
            copy.start()

    barrier = pltpu.get_barrier_semaphore()

    flat = s * width + c

    @pl.loop(1, n * width)
    def _(k):
        other = lax.rem(flat + k, n * width)
        pl.semaphore_signal(
            barrier,
            inc=1,
            device_id={"sp": other // width, "tp": lax.rem(other, width)},
            device_id_type=MESH,
        )

    for b in range(2):

        @pl.when(owners[b] == 0)
        def _(b=b):
            xext[b, pl.ds(0, EDGE), :] = jnp.zeros((EDGE, xext.shape[2]), BF16)

        @pl.when(owners[b] == n - 1)
        def _(b=b):
            xext[b, pl.ds(EDGE + tokens, EDGE), :] = jnp.zeros((EDGE, xext.shape[2]), BF16)

    pl.semaphore_wait(barrier, n * width - 1)

    def swap(k):
        return pltpu.make_async_remote_copy(
            src_ref=x,
            dst_ref=xext.at[0, pl.ds(EDGE, tokens), mine],
            send_sem=sem_x.at[0, k],
            recv_sem=sem_x.at[1, k],
            device_id={"sp": s, "tp": mate(k)},
            device_id_type=MESH,
        )

    def halo(b, up, cross):
        slot = (b * 2 + up) * width + cross
        target = s + 1 if up else s - 1
        return pltpu.make_async_remote_copy(
            src_ref=x.at[pl.ds(tokens - EDGE if up else 0, EDGE), :],
            dst_ref=xext.at[b, pl.ds(0 if up else EDGE + tokens, EDGE), mine],
            send_sem=sem_halo.at[0, slot],
            recv_sem=sem_halo.at[1, slot],
            device_id={
                "sp": target if b == 0 else lax.rem(target + half, n),
                "tp": mate(cross),
            },
            device_id_type=MESH,
        )

    def far(piece):
        return pltpu.make_async_remote_copy(
            src_ref=x.at[pl.ds(piece * SPAN, SPAN), :],
            dst_ref=xext.at[1, pl.ds(EDGE + piece * SPAN, SPAN), mine],
            send_sem=sem_far.at[0, piece],
            recv_sem=sem_far.at[1, piece],
            device_id={"sp": across, "tp": c},
            device_id_type=MESH,
        )

    def hand_on(piece, k):
        at = xext.at[1, pl.ds(EDGE + piece * SPAN, SPAN), mine]
        return pltpu.make_async_remote_copy(
            src_ref=at,
            dst_ref=at,
            send_sem=sem_pass.at[0, piece, k],
            recv_sem=sem_pass.at[1, piece, k],
            device_id={"sp": s, "tp": mate(k)},
            device_id_type=MESH,
        )

    for k in range(1, width):
        swap(k).start()
    for b in range(2):

        @pl.when(s < n - 1)
        def _(b=b):
            for k in range(width):
                halo(b, 1, k).start()

        @pl.when(s > 0)
        def _(b=b):
            for k in range(width):
                halo(b, 0, k).start()

    for piece in range(spans):
        far(piece).start()

    for copy in smalls:
        copy.wait()

    turned = jnp.transpose(q[0].astype(F32))
    turned = jnp.where(side == 0, turned[:HALF], turned[HALF:])
    for g in range(groups):
        qcol[g] = jnp.broadcast_to(turned[:, g : g + 1], (HALF, LANES))

    own.wait()
    for k in range(1, width):
        swap(k).wait_recv()

    offset = jnp.concatenate([bias[0:1, :], bias[1:2, :]], axis=1)
    speed = jnp.concatenate([rate[0:1, :], rate[1:2, :]], axis=1)
    row = lax.broadcasted_iota(jnp.int32, (SPAN, SPAN), 0)
    col = lax.broadcasted_iota(jnp.int32, (SPAN, SPAN), 1)
    later = jnp.where(col > row, 1.0, 0.0).astype(F32)
    earlier = jnp.where(col < row, 1.0, 0.0).astype(F32)
    local = lax.rem(2 * H - c * heads, 2 * H)
    sub = lax.broadcasted_iota(jnp.int32, (8, LANES), 0)

    def weigh(b):
        raw = jnp.dot(xext[b, pl.ds(EDGE, tokens), :], dtw[...], preferred_element_type=F32)
        raw = raw.astype(BF16).astype(F32) + offset
        step = jnp.maximum(raw, 0.0) + jnp.log1p(jnp.exp(-jnp.abs(raw)))
        decay = -(step * speed) / (tokens * n)
        closing = jnp.zeros((8, LANES), F32)
        for j in range(spans):
            part = slice(j * SPAN, (j + 1) * SPAN)
            ahead = jnp.dot(
                later, decay[part], precision=lax.Precision.HIGHEST, preferred_element_type=F32
            )
            behind = jnp.dot(
                earlier, decay[part], precision=lax.Precision.HIGHEST, preferred_element_type=F32
            )
            weight = jnp.exp(jnp.where(low, ahead, behind)) * step[part]
            wts[b * spans + j] = pltpu.roll(weight, local, 1)
            closing = jnp.where(sub == j, jnp.sum(decay[part], axis=0, keepdims=True), closing)
        return closing

    logs[s] = weigh(0)

    def log_copy(k):
        return pltpu.make_async_remote_copy(
            src_ref=logs.at[s],
            dst_ref=logs.at[s],
            send_sem=sem_c.at[0, k],
            recv_sem=sem_c.at[1, k],
            device_id={"sp": peer(k), "tp": c},
            device_id_type=MESH,
        )

    @pl.loop(1, n)
    def _(k):
        log_copy(k).start()

    def halos_in(b):
        @pl.when(owners[b] > 0)
        def _():
            for k in range(width):
                halo(b, 1, k).wait_recv()

        @pl.when(owners[b] < n - 1)
        def _():
            for k in range(width):
                halo(b, 0, k).wait_recv()

    halos_in(0)

    def one_group(b, block, i):
        j = block * (tile // PER) + i
        if b == 0:
            for copy in weight_copies(j):
                copy.wait()
        at_x = pl.ds(pl.multiple_of(j * vcols, vcols), vcols)
        at_b = pl.ds(pl.multiple_of(j * N, N), N)
        rows = xext[b]
        keys = conv_silu(
            jnp.dot(rows, bwv[:, at_b], preferred_element_type=F32), cb[:, at_b].astype(F32), tokens
        )
        values = conv_silu(
            jnp.dot(rows, xwv[:, at_x], preferred_element_type=F32), cx[:, at_x].astype(F32), tokens
        )
        back = lax.rem(LANES - j * PER, LANES)
        for k in range(spans):
            part = slice(k * SPAN, (k + 1) * SPAN)
            turned_keys = jnp.transpose(keys[part])
            turned_keys = jnp.where(side == 0, turned_keys[:HALF], turned_keys[HALF:]).astype(BF16)
            weight = pltpu.roll(wts[b * spans + k], back, 1)
            scaled = []
            for h in range(PER):
                pair = values[part, (h // 2) * LANES : (h // 2 + 1) * LANES]
                other = pltpu.roll(pair, P_SIZE, 1)
                doubled = jnp.where(low, pair, other) if h % 2 == 0 else jnp.where(low, other, pair)
                both = jnp.where(low, weight[:, h : h + 1], weight[:, H + h : H + h + 1])
                scaled.append((doubled * both).astype(BF16))
            states = jnp.dot(
                turned_keys, jnp.concatenate(scaled, axis=1), preferred_element_type=F32
            )
            for h in range(PER):
                state = states[:, h * LANES : (h + 1) * LANES]
                held[k, pl.ds(pl.multiple_of((i * PER + h) * PITCH, 8), HALF), :] = state
                seen = jnp.sum(qcol[j] * state.astype(BF16).astype(F32), axis=0, keepdims=True)
                reads[b * spans + k, pl.ds(j * PER + h, 1), :] = seen

    def goal(b, block):
        at = pl.ds(pl.multiple_of(block * tile, tile), tile)
        return out.at[pl.ds(owners[b] * spans, spans), :, at, :]

    def big_copy(b, block, k):
        return pltpu.make_async_remote_copy(
            src_ref=stage.at[near(k), b, block],
            dst_ref=goal(b, block),
            send_sem=sem_big.at[0, b, block, k],
            recv_sem=sem_big.at[1, b, block, k],
            device_id={"sp": side * half + near(k), "tp": c},
            device_id_type=MESH,
        )

    def self_copy(b, block):
        return pltpu.make_async_copy(
            stage.at[place, b, block], goal(b, block), sem_self.at[b, block]
        )

    def lay_out(b, block, d):
        for k in range(spans):
            for m in range(columns // LANES):
                first = d * (columns // P_SIZE) + 2 * m
                even = held[k, pl.ds(first, tile, stride=PITCH), :]
                odd = held[k, pl.ds(first + 1, tile, stride=PITCH), :]
                at = pl.ds(m * LANES, LANES)
                stage[d, b, block, k, 0, :, at] = jnp.where(
                    low, even, pltpu.roll(odd, P_SIZE, 1)
                ).astype(BF16)
                stage[d, b, block, k, 1, :, at] = jnp.where(
                    low, pltpu.roll(even, P_SIZE, 1), odd
                ).astype(BF16)

    def part_copy(k):
        return pltpu.make_async_remote_copy(
            src_ref=parts.at[s],
            dst_ref=parts.at[s],
            send_sem=sem_y.at[0, k],
            recv_sem=sem_y.at[1, k],
            device_id={"sp": peer(k), "tp": c},
            device_id_type=MESH,
        )

    def send_read():
        @pl.loop(1, n)
        def _(k):
            log_copy(k).wait_recv()

        every = logs[...]
        index = lax.broadcasted_iota(jnp.int32, every.shape, 0) * spans + lax.broadcasted_iota(
            jnp.int32, every.shape, 1
        )
        real = lax.broadcasted_iota(jnp.int32, every.shape, 1) < spans
        r = chosen[0]
        table = jnp.zeros((8, LANES), F32)
        for k in range(2 * spans):
            j = owners[k // spans] * spans + k % spans
            forward = real & (index > j) & (index <= r) & low[None]
            backward = real & (index < j) & (index >= r) & (~low)[None]
            total = jnp.sum(jnp.where(forward | backward, every, 0.0), axis=0)
            total = jnp.sum(total, axis=0, keepdims=True)
            ahead_on = jnp.where(j <= r, 1.0, 0.0)
            behind_on = jnp.where(j >= r, 1.0, 0.0)
            found = jnp.exp(total) * jnp.where(low, ahead_on, behind_on)
            table = jnp.where(sub == k, found, table)
        table = jnp.transpose(pltpu.roll(table, local, 1))
        sums = jnp.zeros((heads, LANES), F32)
        for k in range(2 * spans):
            spread = jnp.where(low, table[0:heads, k : k + 1], table[H : H + heads, k : k + 1])
            sums = sums + spread * reads[k]
        parts[s] = sums

        @pl.loop(1, n)
        def _(k):
            part_copy(k).start()

    def form(b, block):
        @pl.loop(0, tile // PER)
        def _(i):
            one_group(b, block, i)

    def deliver(b, block):
        @pl.loop(1, half)
        def _(k):
            lay_out(b, block, near(k))
            big_copy(b, block, k).start()

        lay_out(b, block, place)
        self_copy(b, block).start()

    @pl.loop(0, blocks)
    def _(block):
        form(0, block)
        deliver(0, block)

    for piece in range(spans):
        far(piece).wait_recv()
        for k in range(1, width):
            hand_on(piece, k).start()
    halos_in(1)
    for piece in range(spans):
        for k in range(1, width):
            hand_on(piece, k).wait_recv()
    weigh(1)

    @pl.loop(0, blocks - 1)
    def _(block):
        form(1, block)
        deliver(1, block)

    form(1, blocks - 1)
    send_read()
    deliver(1, blocks - 1)

    @pl.loop(1, n)
    def _(k):
        part_copy(k).wait_recv()

    def add_part(i, total):
        return total + parts[i]

    total = lax.fori_loop(1, n, add_part, parts[0])
    total = total + pltpu.roll(total, P_SIZE, 1)
    door = gate[0].astype(F32)
    gated = total[:, :P_SIZE] * (door / (1.0 + jnp.exp(-door)))
    squares[c] = jnp.broadcast_to(jnp.sum(gated * gated, keepdims=True), (8, LANES))

    def square(k):
        return pltpu.make_async_remote_copy(
            src_ref=squares.at[c],
            dst_ref=squares.at[c],
            send_sem=sem_sq.at[0, k],
            recv_sem=sem_sq.at[1, k],
            device_id={"sp": s, "tp": mate(k)},
            device_id_type=MESH,
        )

    for k in range(1, width):
        square(k).start()
    for k in range(1, width):
        square(k).wait_recv()
    mean = jnp.sum(squares[...], axis=0)[0:1, 0:1] / (H * P_SIZE)
    fr[0] = (gated * lax.rsqrt(mean + EPSILON) * gain[...]).astype(BF16)

    for k in range(1, width):
        square(k).wait_send()
    for k in range(1, width):
        swap(k).wait_send()

    for b in range(2):

        @pl.when(s < n - 1)
        def _(b=b):
            for k in range(width):
                halo(b, 1, k).wait_send()

        @pl.when(s > 0)
        def _(b=b):
            for k in range(width):
                halo(b, 0, k).wait_send()

    for piece in range(spans):
        far(piece).wait_send()
        for k in range(1, width):
            hand_on(piece, k).wait_send()

    @pl.loop(1, n)
    def _(k):
        log_copy(k).wait_send()
        part_copy(k).wait_send()

    for b in range(2):

        @pl.loop(0, blocks)
        def _(block, b=b):
            self_copy(b, block).wait()

            @pl.loop(1, half)
            def _(k):
                big_copy(b, block, k).wait()


def per_device(x, xw, bw, dtw, bias, rate, cx, cb, q, gate, chosen, gain):
    n = lax.axis_size("sp")
    width = lax.axis_size("tp")
    tokens, feats = x.shape
    depth = xw.shape[0]
    spans = tokens // SPAN
    heads = xw.shape[1] // P_SIZE
    groups = heads // PER
    tile = min(ROWS, heads)
    blocks = heads // tile
    columns = N * P_SIZE // n
    small = (dtw, bias, rate, cx, cb, q, gate, gain)
    vmem = pl.BlockSpec(memory_space=pltpu.VMEM)
    anywhere = pl.BlockSpec(memory_space=pltpu.HBM)
    dma = pltpu.SemaphoreType.DMA
    return pl.pallas_call(
        functools.partial(kernel, n, width),
        out_shape=(
            jax.ShapeDtypeStruct((spans * n, 2, heads, columns), BF16),
            jax.ShapeDtypeStruct((1, heads, P_SIZE), BF16),
        ),
        in_specs=[anywhere] * 10 + [pl.BlockSpec(memory_space=pltpu.SMEM), anywhere],
        out_specs=(vmem, vmem),
        scratch_shapes=[pltpu.VMEM(a.shape, a.dtype) for a in small]
        + [
            pltpu.VMEM((2, tokens + 2 * EDGE, depth), BF16),
            pltpu.VMEM(xw.shape, BF16),
            pltpu.VMEM(bw.shape, BF16),
            pltpu.VMEM((spans, tile * PITCH, LANES), F32),
            pltpu.VMEM((n // 2, 2, blocks, spans, 2, tile, columns), BF16),
            pltpu.VMEM((2 * spans, SPAN, LANES), F32),
            pltpu.VMEM((2 * spans, heads, LANES), F32),
            pltpu.VMEM((groups, HALF, LANES), F32),
            pltpu.VMEM((n, 8, LANES), F32),
            pltpu.VMEM((n, heads, LANES), F32),
            pltpu.VMEM((width, 8, LANES), F32),
            dma((8,)),
            dma((2, groups)),
            dma,
            dma((2, width)),
            dma((2, spans)),
            dma((2, spans, width)),
            dma((2, 4 * width)),
            dma((2, n)),
            dma((2, n)),
            dma((2, 2, blocks, n // 2)),
            dma((2, blocks)),
            dma((2, width)),
        ],
        compiler_params=pltpu.CompilerParams(
            collective_id=0, has_side_effects=True, vmem_limit_bytes=40 * 1024 * 1024
        ),
    )(x, xw, bw, dtw, bias, rate, cx, cb, q, gate, chosen, gain)


def solution(mesh):
    return jax.shard_map(
        per_device,
        mesh=mesh,
        in_specs=(
            P(("gr", "sp"), "tp"),
            P(None, "tp"),
            P(None, "tp"),
            P(),
            P(),
            P(),
            P(None, "tp"),
            P(None, "tp"),
            P("gr", "tp", None),
            P("gr", "tp", None),
            P("gr"),
            P("tp", None),
        ),
        out_specs=(P("gr", None, "tp", "sp"), P("gr", "tp", None)),
        check_vma=False,
    )
```

```python
import functools

import jax
import jax.numpy as jnp
from jax import lax
from jax.experimental import pallas as pl
from jax.experimental.pallas import tpu as pltpu
from jax.sharding import PartitionSpec as P

H = 64
P_SIZE = 64
G = 16
N = 128
KW = 5
SPAN = 128
EPSILON = 1e-06
PER = H // G
EDGE = 16
ROWS = 8
HALF = N // 2
PITCH = HALF + 8
LANES = 128
MESH = pl.DeviceIdType.MESH
F32 = jnp.float32
BF16 = jnp.bfloat16


def conv_silu(projected, taps, tokens):
    rounded = projected.astype(BF16).astype(F32)
    total = rounded.shape[0]
    reach = KW // 2
    mixed = None
    for k in range(KW):
        shift = (reach - k) % total
        moved = rounded if shift == 0 else pltpu.roll(rounded, shift, 0)
        term = taps[k : k + 1] * moved[EDGE : EDGE + tokens]
        mixed = term if mixed is None else mixed + term
    return (mixed / (1.0 + jnp.exp(-mixed))).astype(BF16).astype(F32)


def kernel(
    n, width, x, xw, bw, dtw_h, bias_h, rate_h, cx_h, cb_h, q_h, gate_h, chosen, gain_h,
    out, fr,
    dtw, bias, rate, cx, cb, q, gate, gain,
    xext, xwv, bwv, held, stage, wts, reads, qcol, logs, parts, squares,
    sem_small, sem_w, sem_own, sem_x, sem_far, sem_pass, sem_halo, sem_c, sem_y, sem_big, sem_self, sem_sq,
):
    s = lax.axis_index("sp")
    c = lax.axis_index("tp")
    tokens, feats = x.shape
    spans = tokens // SPAN
    heads = xw.shape[1] // P_SIZE
    groups = heads // PER
    tile = min(ROWS, heads)
    blocks = heads // tile
    vcols = PER * P_SIZE
    columns = stage.shape[-1]
    lane = lax.broadcasted_iota(jnp.int32, (1, LANES), 1)
    low = lane < P_SIZE

    half = n // 2
    side = s // half
    place = lax.rem(s, half)
    across = lax.rem(s + half, n)
    owners = (s, across)

    def peer(k):
        return lax.rem(s + k, n)

    def near(k):
        return lax.rem(place + k, half)

    def mate(k):
        return lax.rem(c + k, width)

    def weight_copies(j):
        at_x = pl.ds(pl.multiple_of(j * vcols, vcols), vcols)
        at_b = pl.ds(pl.multiple_of(j * N, N), N)
        return (
            pltpu.make_async_copy(xw.at[:, at_x], xwv.at[:, at_x], sem_w.at[0, j]),
            pltpu.make_async_copy(bw.at[:, at_b], bwv.at[:, at_b], sem_w.at[1, j]),
        )

    smalls = [
        pltpu.make_async_copy(a, b, sem_small.at[i])
        for i, (a, b) in enumerate(
            (
                (dtw_h, dtw), (bias_h, bias), (rate_h, rate), (cx_h, cx),
                (cb_h, cb), (q_h, q), (gate_h, gate), (gain_h, gain),
            )
        )
    ]
    mine = pl.ds(pl.multiple_of(c * feats, feats), feats)
    own = pltpu.make_async_copy(x, xext.at[0, pl.ds(EDGE, tokens), mine], sem_own)
    own.start()
    for copy in smalls:
        copy.start()
    for j in range(groups):
        for copy in weight_copies(j):
            copy.start()

    barrier = pltpu.get_barrier_semaphore()

    flat = s * width + c

    @pl.loop(1, n * width)
    def _(k):
        other = lax.rem(flat + k, n * width)
        pl.semaphore_signal(
            barrier,
            inc=1,
            device_id={"sp": other // width, "tp": lax.rem(other, width)},
            device_id_type=MESH,
        )

    for b in range(2):

        @pl.when(owners[b] == 0)
        def _(b=b):
            xext[b, pl.ds(0, EDGE), :] = jnp.zeros((EDGE, xext.shape[2]), BF16)

        @pl.when(owners[b] == n - 1)
        def _(b=b):
            xext[b, pl.ds(EDGE + tokens, EDGE), :] = jnp.zeros((EDGE, xext.shape[2]), BF16)

    pl.semaphore_wait(barrier, n * width - 1)

    def swap(k):
        return pltpu.make_async_remote_copy(
            src_ref=x,
            dst_ref=xext.at[0, pl.ds(EDGE, tokens), mine],
            send_sem=sem_x.at[0, k],
            recv_sem=sem_x.at[1, k],
            device_id={"sp": s, "tp": mate(k)},
            device_id_type=MESH,
        )

    def halo(b, up, cross):
        slot = (b * 2 + up) * width + cross
        target = s + 1 if up else s - 1
        return pltpu.make_async_remote_copy(
            src_ref=x.at[pl.ds(tokens - EDGE if up else 0, EDGE), :],
            dst_ref=xext.at[b, pl.ds(0 if up else EDGE + tokens, EDGE), mine],
            send_sem=sem_halo.at[0, slot],
            recv_sem=sem_halo.at[1, slot],
            device_id={
                "sp": target if b == 0 else lax.rem(target + half, n),
                "tp": mate(cross),
            },
            device_id_type=MESH,
        )

    def far(piece):
        return pltpu.make_async_remote_copy(
            src_ref=x.at[pl.ds(piece * SPAN, SPAN), :],
            dst_ref=xext.at[1, pl.ds(EDGE + piece * SPAN, SPAN), mine],
            send_sem=sem_far.at[0, piece],
            recv_sem=sem_far.at[1, piece],
            device_id={"sp": across, "tp": c},
            device_id_type=MESH,
        )

    def hand_on(piece, k):
        at = xext.at[1, pl.ds(EDGE + piece * SPAN, SPAN), mine]
        return pltpu.make_async_remote_copy(
            src_ref=at,
            dst_ref=at,
            send_sem=sem_pass.at[0, piece, k],
            recv_sem=sem_pass.at[1, piece, k],
            device_id={"sp": s, "tp": mate(k)},
            device_id_type=MESH,
        )

    for k in range(1, width):
        swap(k).start()
    for b in range(2):

        @pl.when(s < n - 1)
        def _(b=b):
            for k in range(width):
                halo(b, 1, k).start()

        @pl.when(s > 0)
        def _(b=b):
            for k in range(width):
                halo(b, 0, k).start()

    for piece in range(spans):
        far(piece).start()

    for copy in smalls:
        copy.wait()

    turned = jnp.transpose(q[0].astype(F32))
    turned = jnp.where(side == 0, turned[:HALF], turned[HALF:])
    for g in range(groups):
        qcol[g] = jnp.broadcast_to(turned[:, g : g + 1], (HALF, LANES))

    own.wait()
    for k in range(1, width):
        swap(k).wait_recv()

    offset = jnp.concatenate([bias[0:1, :], bias[1:2, :]], axis=1)
    speed = jnp.concatenate([rate[0:1, :], rate[1:2, :]], axis=1)
    row = lax.broadcasted_iota(jnp.int32, (SPAN, SPAN), 0)
    col = lax.broadcasted_iota(jnp.int32, (SPAN, SPAN), 1)
    later = jnp.where(col > row, 1.0, 0.0).astype(F32)
    earlier = jnp.where(col < row, 1.0, 0.0).astype(F32)
    local = lax.rem(2 * H - c * heads, 2 * H)
    sub = lax.broadcasted_iota(jnp.int32, (8, LANES), 0)

    def weigh(b):
        raw = jnp.dot(xext[b, pl.ds(EDGE, tokens), :], dtw[...], preferred_element_type=F32)
        raw = raw.astype(BF16).astype(F32) + offset
        step = jnp.maximum(raw, 0.0) + jnp.log1p(jnp.exp(-jnp.abs(raw)))
        decay = -(step * speed) / (tokens * n)
        closing = jnp.zeros((8, LANES), F32)
        for j in range(spans):
            part = slice(j * SPAN, (j + 1) * SPAN)
            ahead = jnp.dot(
                later, decay[part], precision=lax.Precision.HIGHEST, preferred_element_type=F32
            )
            behind = jnp.dot(
                earlier, decay[part], precision=lax.Precision.HIGHEST, preferred_element_type=F32
            )
            weight = jnp.exp(jnp.where(low, ahead, behind)) * step[part]
            wts[b * spans + j] = pltpu.roll(weight, local, 1)
            closing = jnp.where(sub == j, jnp.sum(decay[part], axis=0, keepdims=True), closing)
        return closing

    logs[s] = weigh(0)

    def log_copy(k):
        return pltpu.make_async_remote_copy(
            src_ref=logs.at[s],
            dst_ref=logs.at[s],
            send_sem=sem_c.at[0, k],
            recv_sem=sem_c.at[1, k],
            device_id={"sp": peer(k), "tp": c},
            device_id_type=MESH,
        )

    @pl.loop(1, n)
    def _(k):
        log_copy(k).start()

    def halos_in(b):
        @pl.when(owners[b] > 0)
        def _():
            for k in range(width):
                halo(b, 1, k).wait_recv()

        @pl.when(owners[b] < n - 1)
        def _():
            for k in range(width):
                halo(b, 0, k).wait_recv()

    halos_in(0)

    pack = tile // PER

    def form(b, block):
        if b == 0:
            for i in range(pack):
                for copy in weight_copies(block * pack + i):
                    copy.wait()
        at_x = pl.ds(pl.multiple_of(block * pack * vcols, pack * vcols), pack * vcols)
        at_b = pl.ds(pl.multiple_of(block * pack * N, pack * N), pack * N)
        rows = xext[b]
        all_keys = conv_silu(
            jnp.dot(rows, bwv[:, at_b], preferred_element_type=F32), cb[:, at_b].astype(F32), tokens
        )
        all_values = conv_silu(
            jnp.dot(rows, xwv[:, at_x], preferred_element_type=F32), cx[:, at_x].astype(F32), tokens
        )
        for i in range(pack):
            one_group(
                b,
                block * pack + i,
                i,
                all_keys[:, i * N : (i + 1) * N],
                all_values[:, i * vcols : (i + 1) * vcols],
            )

    def one_group(b, j, i, keys, values):
        back = lax.rem(LANES - j * PER, LANES)
        for k in range(spans):
            part = slice(k * SPAN, (k + 1) * SPAN)
            turned_keys = jnp.transpose(keys[part])
            turned_keys = jnp.where(side == 0, turned_keys[:HALF], turned_keys[HALF:]).astype(BF16)
            weight = pltpu.roll(wts[b * spans + k], back, 1)
            scaled = []
            for h in range(PER):
                pair = values[part, (h // 2) * LANES : (h // 2 + 1) * LANES]
                other = pltpu.roll(pair, P_SIZE, 1)
                doubled = jnp.where(low, pair, other) if h % 2 == 0 else jnp.where(low, other, pair)
                both = jnp.where(low, weight[:, h : h + 1], weight[:, H + h : H + h + 1])
                scaled.append((doubled * both).astype(BF16))
            states = jnp.dot(
                turned_keys, jnp.concatenate(scaled, axis=1), preferred_element_type=F32
            )
            for h in range(PER):
                state = states[:, h * LANES : (h + 1) * LANES]
                held[k, pl.ds((i * PER + h) * PITCH, HALF), :] = state
                seen = jnp.sum(qcol[j] * state.astype(BF16).astype(F32), axis=0, keepdims=True)
                reads[b * spans + k, pl.ds(j * PER + h, 1), :] = seen

    def goal(b, block):
        at = pl.ds(pl.multiple_of(block * tile, tile), tile)
        return out.at[pl.ds(owners[b] * spans, spans), :, at, :]

    def big_copy(b, block, k):
        return pltpu.make_async_remote_copy(
            src_ref=stage.at[near(k), b, block],
            dst_ref=goal(b, block),
            send_sem=sem_big.at[0, b, block, k],
            recv_sem=sem_big.at[1, b, block, k],
            device_id={"sp": side * half + near(k), "tp": c},
            device_id_type=MESH,
        )

    def self_copy(b, block):
        return pltpu.make_async_copy(
            stage.at[place, b, block], goal(b, block), sem_self.at[b, block]
        )

    def lay_out(b, block, d):
        for k in range(spans):
            for m in range(columns // LANES):
                first = d * (columns // P_SIZE) + 2 * m
                even = held[k, pl.ds(first, tile, stride=PITCH), :]
                odd = held[k, pl.ds(first + 1, tile, stride=PITCH), :]
                at = pl.ds(m * LANES, LANES)
                stage[d, b, block, k, 0, :, at] = jnp.where(
                    low, even, pltpu.roll(odd, P_SIZE, 1)
                ).astype(BF16)
                stage[d, b, block, k, 1, :, at] = jnp.where(
                    low, pltpu.roll(even, P_SIZE, 1), odd
                ).astype(BF16)

    def part_copy(k):
        return pltpu.make_async_remote_copy(
            src_ref=parts.at[s],
            dst_ref=parts.at[s],
            send_sem=sem_y.at[0, k],
            recv_sem=sem_y.at[1, k],
            device_id={"sp": peer(k), "tp": c},
            device_id_type=MESH,
        )

    def send_read():
        @pl.loop(1, n)
        def _(k):
            log_copy(k).wait_recv()

        every = logs[...]
        index = lax.broadcasted_iota(jnp.int32, every.shape, 0) * spans + lax.broadcasted_iota(
            jnp.int32, every.shape, 1
        )
        real = lax.broadcasted_iota(jnp.int32, every.shape, 1) < spans
        r = chosen[0]
        table = jnp.zeros((8, LANES), F32)
        for k in range(2 * spans):
            j = owners[k // spans] * spans + k % spans
            forward = real & (index > j) & (index <= r) & low[None]
            backward = real & (index < j) & (index >= r) & (~low)[None]
            total = jnp.sum(jnp.where(forward | backward, every, 0.0), axis=0)
            total = jnp.sum(total, axis=0, keepdims=True)
            ahead_on = jnp.where(j <= r, 1.0, 0.0)
            behind_on = jnp.where(j >= r, 1.0, 0.0)
            found = jnp.exp(total) * jnp.where(low, ahead_on, behind_on)
            table = jnp.where(sub == k, found, table)
        table = jnp.transpose(pltpu.roll(table, local, 1))
        sums = jnp.zeros((heads, LANES), F32)
        for k in range(2 * spans):
            spread = jnp.where(low, table[0:heads, k : k + 1], table[H : H + heads, k : k + 1])
            sums = sums + spread * reads[k]
        parts[s] = sums

        @pl.loop(1, n)
        def _(k):
            part_copy(k).start()

    def deliver(b, block):
        @pl.loop(1, half)
        def _(k):
            lay_out(b, block, near(k))
            big_copy(b, block, k).start()

        lay_out(b, block, place)
        self_copy(b, block).start()

    @pl.loop(0, blocks)
    def _(block):
        form(0, block)
        deliver(0, block)

    for piece in range(spans):
        far(piece).wait_recv()
        for k in range(1, width):
            hand_on(piece, k).start()
    halos_in(1)
    for piece in range(spans):
        for k in range(1, width):
            hand_on(piece, k).wait_recv()
    weigh(1)

    @pl.loop(0, blocks - 1)
    def _(block):
        form(1, block)
        deliver(1, block)

    form(1, blocks - 1)
    send_read()
    deliver(1, blocks - 1)

    @pl.loop(1, n)
    def _(k):
        part_copy(k).wait_recv()

    def add_part(i, total):
        return total + parts[i]

    total = lax.fori_loop(1, n, add_part, parts[0])
    total = total + pltpu.roll(total, P_SIZE, 1)
    door = gate[0].astype(F32)
    gated = total[:, :P_SIZE] * (door / (1.0 + jnp.exp(-door)))
    squares[c] = jnp.broadcast_to(jnp.sum(gated * gated, keepdims=True), (8, LANES))

    def square(k):
        return pltpu.make_async_remote_copy(
            src_ref=squares.at[c],
            dst_ref=squares.at[c],
            send_sem=sem_sq.at[0, k],
            recv_sem=sem_sq.at[1, k],
            device_id={"sp": s, "tp": mate(k)},
            device_id_type=MESH,
        )

    for k in range(1, width):
        square(k).start()
    for k in range(1, width):
        square(k).wait_recv()
    mean = jnp.sum(squares[...], axis=0)[0:1, 0:1] / (H * P_SIZE)
    fr[0] = (gated * lax.rsqrt(mean + EPSILON) * gain[...]).astype(BF16)

    for k in range(1, width):
        square(k).wait_send()
    for k in range(1, width):
        swap(k).wait_send()

    for b in range(2):

        @pl.when(s < n - 1)
        def _(b=b):
            for k in range(width):
                halo(b, 1, k).wait_send()

        @pl.when(s > 0)
        def _(b=b):
            for k in range(width):
                halo(b, 0, k).wait_send()

    for piece in range(spans):
        far(piece).wait_send()
        for k in range(1, width):
            hand_on(piece, k).wait_send()

    @pl.loop(1, n)
    def _(k):
        log_copy(k).wait_send()
        part_copy(k).wait_send()

    for b in range(2):

        @pl.loop(0, blocks)
        def _(block, b=b):
            self_copy(b, block).wait()

            @pl.loop(1, half)
            def _(k):
                big_copy(b, block, k).wait()


def per_device(x, xw, bw, dtw, bias, rate, cx, cb, q, gate, chosen, gain):
    n = lax.axis_size("sp")
    width = lax.axis_size("tp")
    tokens, feats = x.shape
    depth = xw.shape[0]
    spans = tokens // SPAN
    heads = xw.shape[1] // P_SIZE
    groups = heads // PER
    tile = min(ROWS, heads)
    blocks = heads // tile
    columns = N * P_SIZE // n
    small = (dtw, bias, rate, cx, cb, q, gate, gain)
    vmem = pl.BlockSpec(memory_space=pltpu.VMEM)
    anywhere = pl.BlockSpec(memory_space=pl.ANY)
    dma = pltpu.SemaphoreType.DMA
    return pl.pallas_call(
        functools.partial(kernel, n, width),
        out_shape=(
            jax.ShapeDtypeStruct((spans * n, 2, heads, columns), BF16),
            jax.ShapeDtypeStruct((1, heads, P_SIZE), BF16),
        ),
        in_specs=[anywhere] * 10 + [pl.BlockSpec(memory_space=pltpu.SMEM), anywhere],
        out_specs=(anywhere, vmem),
        scratch_shapes=[pltpu.VMEM(a.shape, a.dtype) for a in small]
        + [
            pltpu.VMEM((2, tokens + 2 * EDGE, depth), BF16),
            pltpu.VMEM(xw.shape, BF16),
            pltpu.VMEM(bw.shape, BF16),
            pltpu.VMEM((spans, tile * PITCH, LANES), F32),
            pltpu.VMEM((n // 2, 2, blocks, spans, 2, tile, columns), BF16),
            pltpu.VMEM((2 * spans, SPAN, LANES), F32),
            pltpu.VMEM((2 * spans, heads, LANES), F32),
            pltpu.VMEM((groups, HALF, LANES), F32),
            pltpu.VMEM((n, 8, LANES), F32),
            pltpu.VMEM((n, heads, LANES), F32),
            pltpu.VMEM((width, 8, LANES), F32),
            dma((8,)),
            dma((2, groups)),
            dma,
            dma((2, width)),
            dma((2, spans)),
            dma((2, spans, width)),
            dma((2, 4 * width)),
            dma((2, n)),
            dma((2, n)),
            dma((2, 2, blocks, n // 2)),
            dma((2, blocks)),
            dma((2, width)),
        ],
        compiler_params=pltpu.CompilerParams(
            collective_id=0, has_side_effects=True, vmem_limit_bytes=56 * 1024 * 1024
        ),
    )(x, xw, bw, dtw, bias, rate, cx, cb, q, gate, chosen, gain)


def solution(mesh):
    return jax.shard_map(
        per_device,
        mesh=mesh,
        in_specs=(
            P(("gr", "sp"), "tp"),
            P(None, "tp"),
            P(None, "tp"),
            P(),
            P(),
            P(),
            P(None, "tp"),
            P(None, "tp"),
            P("gr", "tp", None),
            P("gr", "tp", None),
            P("gr"),
            P("tp", None),
        ),
        out_specs=(P("gr", None, "tp", "sp"), P("gr", "tp", None)),
        check_vma=False,
    )
```
